128 devices in a mesh: ep: 128 (over z, y, x, core).
Axes of the slice: x: 4, y: 4, z: 4, core: 2. Of those that a mesh axis runs over, the one named last changes fastest.
Arguments:
- tokens: bfloat16 [1024, 2048], P('ep'), may hold values from -6 to 6
- cache_keys: bfloat16 [1024, 1024, 128], P('ep'), may hold values from -80 to 80
- cache_values: bfloat16 [1024, 1024, 128], P('ep'), may hold values from -6 to 6
- cum_gates: float32 [1024, 1024, 2], P('ep'), may hold values from -1024 to 0, as said below
- lengths: int32 [1024], P('ep'), may hold values from 128 to 1024
- query_weight: bfloat16 [2048, 2048], replicated, may hold values from -0.125 to 0.125
- key_weight: bfloat16 [2048, 128], replicated, may hold values from -0.125 to 0.125
- value_weight: bfloat16 [2048, 128], replicated, may hold values from -0.125 to 0.125
- forget_weight: bfloat16 [2048, 2], replicated, may hold values from -0.125 to 0.125
- out_weight: bfloat16 [2048, 2048], P('ep'), may hold values from -1 to 1
- norm_gain: float32 [2, 2048], replicated, may hold values from 0.1 to 1.9
- norm_bias: float32 [2, 2048], replicated, may hold values from -1 to 1
- dense_gate_weight: bfloat16 [2048, 5632], P(None, 'ep'), may hold values from -0.125 to 0.125
- dense_up_weight: bfloat16 [2048, 5632], P(None, 'ep'), may hold values from -0.125 to 0.125
- dense_down_weight: bfloat16 [5632, 2048], P('ep'), may hold values from -0.078125 to 0.078125
- dense_scale: float32 [2048], replicated, may hold values from 0.2 to 1.5
- expert_gate_weight: bfloat16 [2048, 57344], P(None, 'ep'), may hold values from -0.125 to 0.125
- expert_up_weight: bfloat16 [2048, 57344], P(None, 'ep'), may hold values from -0.125 to 0.125
- expert_down_weight: bfloat16 [57344, 2048], P('ep'), may hold values from -0.0625 to 0.0625
- routes: int32 [1024, 2], replicated, may hold values from 0 to 7, all different within a row; in each aligned block of 8 rows (0 to 7, 8 to 15, ...) at most 3 rows name the same one
- route_weights: float32 [1024, 2], replicated, may hold values from 0.2 to 1
Outputs:
- output: bfloat16 [1024, 2048], P('ep')
The draws below stay inside these ranges and needn't reach their ends.
Inputs may be any that keep to these rules, and one draw needn't show every extreme that they name: `routes`: each row names 2 different experts; the rows of one device (8 aligned rows) name one expert at most 3 times. `cum_gates`: non-increasing along positions.
All inputs are finite; a program needn't handle non-finite values.
Results may differ from the reference program's by a relative error of at most 0.012.
Values may be sent and summed in bfloat16 or wider, within the bound.
A program may use at most 128 MiB of HBM per device.

```python
import math
import jax
import jax.numpy as jnp
import numpy as np
from jax import lax

D = 2048
HEADS = 32
HEAD_DIM = 64
KEY_VALUE_HEADS = 2
FF_DENSE = 5632
FF_EXPERT = 7168
EXPERTS = 8
TOP = 2
SEQ_DEV = 8
CACHE_SLOTS = 1024
SEQUENCE_COUNT = 1024
CAP = 3
N_EP = 128


def draw_cache_keys(key, part):
    key_rows = jax.random.split(key, 1)
    shape = (SEQUENCE_COUNT, CACHE_SLOTS, KEY_VALUE_HEADS * HEAD_DIM)
    return jax.random.normal(key_rows[0], shape, jnp.float32).astype(jnp.bfloat16)


def draw_cum_gates(key, part):
    key_rows = jax.random.split(key, 7)
    devices = SEQUENCE_COUNT // SEQ_DEV
    share_fast = 0.5
    fast = jax.random.uniform(key_rows[0], (SEQUENCE_COUNT, 1, KEY_VALUE_HEADS)) < share_fast
    fast_rate = jnp.exp(jax.random.uniform(key_rows[1], (SEQUENCE_COUNT, 1, KEY_VALUE_HEADS), jnp.float32, math.log(1.0 / 100.0), math.log(1.0 / 30.0)))
    slow_rate = jnp.exp(jax.random.uniform(key_rows[2], (SEQUENCE_COUNT, 1, KEY_VALUE_HEADS), jnp.float32, math.log(0.1), math.log(0.4))) / CACHE_SLOTS
    decay_rate = jnp.where(fast, fast_rate, slow_rate)
    per_device_ratio = jnp.exp(jax.random.uniform(key_rows[3], (devices, 1, 1), jnp.float32, 0.0, math.log(3.0)))
    per_device_ratio = jnp.repeat(per_device_ratio, SEQ_DEV, axis=0)
    coarse_estimate = jnp.exp(jax.random.uniform(key_rows[4], (SEQUENCE_COUNT, CACHE_SLOTS, KEY_VALUE_HEADS), jnp.float32, math.log(0.5), math.log(2.0)))
    spike_position = jax.random.randint(key_rows[5], (SEQUENCE_COUNT, 1, KEY_VALUE_HEADS, 2), 0, CACHE_SLOTS)
    decay_penalty = jax.random.uniform(key_rows[6], (SEQUENCE_COUNT, 1, KEY_VALUE_HEADS, 2), jnp.float32, 0.2, 0.5)
    current_slot = jnp.arange(CACHE_SLOTS, dtype=jnp.int32)[None, :, None, None]
    spike_amount = jnp.sum(jnp.where(current_slot == spike_position, -jnp.log(1.0 - decay_penalty), 0.0), axis=3)
    step_total = decay_rate * per_device_ratio * coarse_estimate + spike_amount
    return jnp.cumsum(-step_total, axis=1).astype(jnp.float32)


def with_ends(result, key, least, largest):
    longest = result.shape.index(max(result.shape))
    spots = []
    for shift in (0, 1):
        where = [jax.random.randint(jax.random.fold_in(key, axis), (), 0, length) for axis, length in enumerate(result.shape)]
        where[longest] = (where[longest] + shift) % result.shape[longest]
        spots.append(tuple(where))
    return result.at[spots[0]].set(least).at[spots[1]].set(largest)


def levels(stream_key, dims, cuts, smallest, top_value):
    level, own = 1.0, jax.random.fold_in(stream_key, 6)
    for dim, parts in cuts:
        heights = jnp.exp(jax.random.uniform(jax.random.fold_in(own, dim), (parts,), jnp.float32, smallest / len(cuts), top_value / len(cuts)))
        level = level * jnp.repeat(heights, dims[dim] // parts).reshape([-1 if axis == dim else 1 for axis in range(len(dims))])
    return level


def routed_block(stream_key, own, number, rows, count, top, reach, slope):
    ranking = jax.random.permutation(stream_key, count)
    crowded, common = load_shares(count, rows * top, reach, slope, True), load_shares(count, rows * top, reach, slope, False)
    places = jnp.arange(count)

    def named(tallies, turn):
        used = int((tallies > 0).sum())
        fixed = max(1, used // 4)
        shifted = fixed + (places - fixed + turn * (used - fixed)) % max(1, count - fixed)
        return jnp.zeros((count,), jnp.int32).at[ranking[jnp.where(places < fixed, places, shifted)]].set(jnp.asarray(tallies, jnp.int32))

    tallies = jnp.where(number % 4 == 0, named(crowded, number // 4), named(common, number - number // 4 - 1))
    mixed = jax.random.permutation(jax.random.fold_in(own, 3), count)
    source_of, taker = mixed[0:count // 2 * 2:2], mixed[1:count // 2 * 2:2]
    slack = jnp.minimum(tallies[source_of] - 1, reach - tallies[taker]) // 2
    slack = jnp.where((source_of == ranking[0]) | (taker == ranking[0]) | (tallies[taker] == 0), 0, jnp.maximum(slack, 0))
    shifted = jax.random.randint(jax.random.fold_in(own, 4), (count // 2,), 0, 1 << 20) % (slack + 1)
    tallies = tallies.at[source_of].add(-shifted).at[taker].add(shifted)
    items = jnp.searchsorted(jnp.cumsum(tallies), jnp.arange(rows * top), side="right").astype(jnp.int32)
    table = items.reshape(top, rows).T
    table = table[jax.random.permutation(jax.random.fold_in(own, 1), rows)]
    turn = jax.random.randint(jax.random.fold_in(own, 2), (rows, 1), 0, top)
    return jnp.take_along_axis(table, (jnp.arange(top)[None, :] + turn) % top, axis=1)


def load_shares(count, total, bound, skew, full):
    weights = [(1 << 20) // math.isqrt(rank ** skew) + 1 for rank in range(1, count + 1)]
    largest = bound if full else min(bound, max(-(-total // count), total * weights[0] // sum(weights)))
    least = 1 if total - largest >= count - 1 else 0
    holding, spare = [largest] + [least] * (count - 1), total - largest - least * (count - 1)
    while spare > 0:
        movable = [i for i in range(1, count) if holding[i] < largest] or [i for i in range(1, count) if holding[i] < bound]
        whole, remaining = sum([weights[i] for i in movable]), spare
        for i in movable:
            more = min(bound - holding[i], max(1, remaining * weights[i] // whole), spare)
            holding[i] = holding[i] + more
            spare = spare - more
    return np.array(holding)


def normal_values(stream_key, shape, scale, reach, cuts=(), held_as=jnp.bfloat16):
    level = levels(stream_key, shape, cuts, -0.22, 0.18) if cuts else 1.0
    values = jax.random.normal(stream_key, shape, jnp.float32) * scale * level
    return jnp.minimum(jnp.maximum(values, -reach), reach).astype(held_as)


def setup_inputs(seed: int = 0) -> dict:
    keys = jax.random.split(jax.random.key(seed), 22)
    tokens = normal_values(keys[0], (SEQUENCE_COUNT, D), 1.0, 6.0, ((0, 128),))
    cache_keys = draw_cache_keys(jax.random.fold_in(keys[21], 71), 0)
    cache_values = normal_values(keys[2], (SEQUENCE_COUNT, CACHE_SLOTS, KEY_VALUE_HEADS * HEAD_DIM), 1.0, 6.0, ((0, 128),))
    cum_gates = draw_cum_gates(jax.random.fold_in(keys[21], 71), 0)
    lengths = with_ends(jax.random.randint(keys[4], (SEQUENCE_COUNT,), CACHE_SLOTS // 8, CACHE_SLOTS + 1), jax.random.fold_in(keys[4], 1), CACHE_SLOTS // 8, CACHE_SLOTS).astype(jnp.int32)
    query_weight = normal_values(keys[5], (D, HEADS * HEAD_DIM), D ** -0.5, 0.125)
    key_weight = normal_values(keys[6], (D, KEY_VALUE_HEADS * HEAD_DIM), D ** -0.5, 0.125)
    value_weight = normal_values(keys[7], (D, KEY_VALUE_HEADS * HEAD_DIM), D ** -0.5, 0.125)
    forget_weight = normal_values(keys[8], (D, KEY_VALUE_HEADS), D ** -0.5, 0.125)
    out_weight = normal_values(keys[9], (HEADS * HEAD_DIM, D), (HEADS * HEAD_DIM // 64) ** -0.5, 1.0, ((0, 128),))
    norm_gain = jnp.clip(1.0 + 0.18 * jax.random.normal(keys[10], (2, D), jnp.float32), 0.1, 1.9)
    norm_bias = normal_values(keys[11], (2, D), 0.2, 1.0, (), jnp.float32)
    dense_gate_weight = normal_values(keys[12], (D, FF_DENSE), D ** -0.5, 0.125, ((1, 128),))
    dense_up_weight = normal_values(keys[13], (D, FF_DENSE), D ** -0.5, 0.125, ((1, 128),))
    dense_down_weight = normal_values(keys[14], (FF_DENSE, D), FF_DENSE ** -0.5, 0.078125, ((0, 128),))
    dense_scale = jnp.clip(jax.random.uniform(keys[15], (D,), jnp.float32, 0.2, 1.5), 0.2, 1.5)
    expert_gate_weight = normal_values(keys[16], (D, EXPERTS * FF_EXPERT), D ** -0.5, 0.125, ((1, 128),))
    expert_up_weight = normal_values(keys[17], (D, EXPERTS * FF_EXPERT), D ** -0.5, 0.125, ((1, 128),))
    expert_down_weight = normal_values(keys[18], (EXPERTS * FF_EXPERT, D), FF_EXPERT ** -0.5, 0.0625, ((0, 128),))
    routes_keys = jax.random.split(jax.random.fold_in(keys[19], 1), SEQUENCE_COUNT // SEQ_DEV)
    routes_turns = jax.random.permutation(jax.random.fold_in(keys[19], 3), SEQUENCE_COUNT // SEQ_DEV)
    routes = jax.vmap(lambda own, number: routed_block(jax.random.fold_in(keys[19], 2), own, number, SEQ_DEV, EXPERTS, TOP, CAP, 2))(routes_keys, routes_turns).reshape((SEQUENCE_COUNT, TOP))
    route_weights = jnp.clip(jax.random.uniform(keys[20], (SEQUENCE_COUNT, TOP), jnp.float32, 0.2, 1.0), 0.2, 1.0)
    return dict(tokens=tokens, cache_keys=cache_keys, cache_values=cache_values, cum_gates=cum_gates, lengths=lengths, query_weight=query_weight, key_weight=key_weight, value_weight=value_weight, forget_weight=forget_weight, out_weight=out_weight, norm_gain=norm_gain, norm_bias=norm_bias, dense_gate_weight=dense_gate_weight, dense_up_weight=dense_up_weight, dense_down_weight=dense_down_weight, dense_scale=dense_scale, expert_gate_weight=expert_gate_weight, expert_up_weight=expert_up_weight, expert_down_weight=expert_down_weight, routes=routes, route_weights=route_weights)


residual_scale = 1.4142135
norm_eps = 1e-05

def layer_norm(values, gain_row, shift_row):
    centre = lax.optimization_barrier(jnp.mean(values, axis=-1, keepdims=True))
    centred = values - centre
    spread = lax.optimization_barrier(jnp.mean(centred * centred, axis=-1, keepdims=True))
    return (centred * lax.rsqrt(spread + norm_eps) * gain_row + shift_row).astype(jnp.bfloat16)

def attend_block(inputs):
    queries, cached_keys, cached_values, gate_sums, length_row, fresh_key, fresh_value, fresh_gate = inputs
    amount = queries.shape[0]
    grouped = HEADS // KEY_VALUE_HEADS
    query_grid_four = queries.astype(jnp.float32).reshape(amount, KEY_VALUE_HEADS, grouped, HEAD_DIM)
    key_four = cached_keys.astype(jnp.float32).reshape(amount, CACHE_SLOTS, KEY_VALUE_HEADS, HEAD_DIM)
    value_four = cached_values.astype(jnp.float32).reshape(amount, CACHE_SLOTS, KEY_VALUE_HEADS, HEAD_DIM)
    self_key_row = fresh_key.astype(jnp.float32).reshape(amount, KEY_VALUE_HEADS, HEAD_DIM)
    own_value = fresh_value.astype(jnp.float32).reshape(amount, KEY_VALUE_HEADS, HEAD_DIM)
    ratio_value = HEAD_DIM ** (-0.5)
    latest = jnp.take_along_axis(gate_sums, (length_row - 1).astype(jnp.int32)[:, None, None], axis=1)
    offsets = jnp.transpose(latest - gate_sums + fresh_gate[:, None, :], (0, 2, 1))
    past = jnp.einsum('bkgd,blkd->bkgl', query_grid_four, key_four) * ratio_value + offsets[:, :, None, :]
    live = jnp.arange(CACHE_SLOTS, dtype=jnp.int32)[None, :] < length_row[:, None]
    past = jnp.where(live[:, None, None, :], past, -jnp.inf)
    self_part = jnp.einsum('rifs,ris->rif', query_grid_four, self_key_row) * ratio_value
    highest = jnp.maximum(lax.optimization_barrier(jnp.max(past, axis=-1)), self_part)
    past_exp = jnp.exp(past - highest[..., None])
    own_exp = jnp.exp(self_part - highest)
    denominator = lax.optimization_barrier(jnp.sum(past_exp, axis=-1)) + own_exp
    past_weight = lax.optimization_barrier((past_exp / denominator[..., None]).astype(jnp.bfloat16)).astype(jnp.float32)
    own_weight = lax.optimization_barrier((own_exp / denominator).astype(jnp.bfloat16)).astype(jnp.float32)
    mixed = jnp.einsum('bkgl,blkd->bkgd', past_weight, value_four) + own_weight[..., None] * own_value[:, :, None, :]
    return mixed.reshape(amount, HEADS * HEAD_DIM).astype(jnp.bfloat16)

def expert_mix(settled, expert_gate, expert_up, expert_down, routes, route_weights):
    shards = N_EP // EXPERTS
    part_width = FF_EXPERT // shards
    chosen = routes.reshape(N_EP, SEQ_DEV, TOP)
    shares = route_weights.reshape(N_EP, SEQ_DEV, TOP)
    expert_ids = jnp.arange(EXPERTS, dtype=jnp.int32)
    picked = (chosen[..., None] == expert_ids).astype(jnp.int32)
    hits = lax.optimization_barrier(jnp.sum(picked, axis=2))
    portion = lax.optimization_barrier(jnp.sum(picked.astype(jnp.float32) * shares[..., None], axis=2))
    ranks = jnp.cumsum(hits, axis=1) - hits
    slot_ids = jnp.arange(CAP, dtype=jnp.int32)
    matched = (hits[..., None] * (ranks[..., None] == slot_ids).astype(jnp.int32)).astype(jnp.float32)
    by_source = settled.astype(jnp.float32).reshape(N_EP, SEQ_DEV, D)

    def one_expert(running, expert):
        select = lax.dynamic_index_in_dim(matched, expert, 2, keepdims=False)
        weight_here = lax.dynamic_index_in_dim(portion, expert, 2, keepdims=False)
        slot_rows = jnp.einsum('nsc,nsd->ncd', select, by_source, precision=lax.Precision.HIGHEST)
        slot_rows = slot_rows.reshape(N_EP * CAP, D).astype(jnp.bfloat16)
        gate_cols = lax.dynamic_slice_in_dim(expert_gate, expert * FF_EXPERT, FF_EXPERT, 1)
        up_cols = lax.dynamic_slice_in_dim(expert_up, expert * FF_EXPERT, FF_EXPERT, 1)
        down_rows = lax.dynamic_slice_in_dim(expert_down, expert * FF_EXPERT, FF_EXPERT, 0)
        gate_val = jnp.dot(slot_rows, gate_cols, preferred_element_type=jnp.float32)
        up_val = jnp.dot(slot_rows, up_cols, preferred_element_type=jnp.float32)
        hidden = (jax.nn.silu(gate_val) * up_val).astype(jnp.bfloat16)
        pieces = jnp.einsum('rgf,gfd->rgd', hidden.astype(jnp.float32).reshape(N_EP * CAP, shards, part_width), down_rows.astype(jnp.float32).reshape(shards, part_width, D))
        pieces = lax.optimization_barrier(pieces.astype(jnp.bfloat16)).astype(jnp.float32)
        summed = lax.optimization_barrier(jnp.sum(pieces, axis=1)).reshape(N_EP, CAP, D)
        placed = jnp.einsum('nsc,ncd->nsd', select, summed, precision=lax.Precision.HIGHEST)
        return (running + weight_here[..., None] * placed, None)
    combined, unused = lax.scan(one_expert, jnp.zeros((N_EP, SEQ_DEV, D), jnp.float32), jnp.arange(EXPERTS, dtype=jnp.int32))
    return combined.reshape(N_EP * SEQ_DEV, D)

def reference(tokens, cache_keys, cache_values, cum_gates, lengths, query_weight, key_weight, value_weight, forget_weight, out_weight, norm_gain, norm_bias, dense_gate_weight, dense_up_weight, dense_down_weight, dense_scale, expert_gate_weight, expert_up_weight, expert_down_weight, routes, route_weights):
    query = jnp.dot(tokens, query_weight, preferred_element_type=jnp.float32).astype(jnp.bfloat16)
    new_key = jnp.dot(tokens, key_weight, preferred_element_type=jnp.float32).astype(jnp.bfloat16)
    new_value = jnp.dot(tokens, value_weight, preferred_element_type=jnp.float32).astype(jnp.bfloat16)
    new_gate = jax.nn.log_sigmoid(jnp.dot(tokens, forget_weight, preferred_element_type=jnp.float32))

    def blocks(array):
        return array.reshape((N_EP, SEQ_DEV) + array.shape[1:])
    attended = lax.map(attend_block, (blocks(query), blocks(cache_keys), blocks(cache_values), blocks(cum_gates), blocks(lengths), blocks(new_key), blocks(new_value), blocks(new_gate)))
    attended = attended.reshape(SEQUENCE_COUNT, HEADS * HEAD_DIM)
    projected = jnp.dot(attended, out_weight, preferred_element_type=jnp.float32)
    settled = layer_norm(residual_scale * tokens.astype(jnp.float32) + projected, norm_gain[0], norm_bias[0])
    dense_gate = jnp.dot(settled, dense_gate_weight, preferred_element_type=jnp.float32)
    dense_up = jnp.dot(settled, dense_up_weight, preferred_element_type=jnp.float32)
    dense_hidden = (jax.nn.silu(dense_gate) * dense_up).astype(jnp.bfloat16)
    dense_out = jnp.dot(dense_hidden, dense_down_weight, preferred_element_type=jnp.float32)
    expert_out = expert_mix(settled, expert_gate_weight, expert_up_weight, expert_down_weight, routes, route_weights)
    ffn = expert_out + dense_scale * dense_out
    return layer_norm(residual_scale * settled.astype(jnp.float32) + ffn, norm_gain[1], norm_bias[1])
```

```python
import functools
import jax
import jax.numpy as jnp
from jax import lax
from jax.experimental import pallas as pl
from jax.experimental.pallas import tpu as pltpu
from jax.sharding import PartitionSpec as P

EXPERTS = 8
RING = 4
AXES = 3
MESH = pl.DeviceIdType.MESH

residual_scale = 1.4142135
norm_eps = 1e-05


def layer_norm(values, gain_row, shift_row):
    centre = jnp.mean(values, axis=-1, keepdims=True)
    centred = values - centre
    spread = jnp.mean(centred * centred, axis=-1, keepdims=True)
    return (centred * lax.rsqrt(spread + norm_eps) * gain_row + shift_row).astype(jnp.bfloat16)


def attend(
    heads, kv_count, tokens_ref, query_weight_ref, key_weight_ref, value_weight_ref,
    forget_ref, keys_ref, values_ref, gates_ref, lengths_ref, query_ref, rows_ref, waits,
):
    seqs, model = tokens_ref.shape
    width = key_weight_ref.shape[1]
    head_dim = width // kv_count
    grouped = heads // kv_count
    cache_len = keys_ref.shape[1]
    ratio_value = head_dim ** (-0.5)
    tokens = tokens_ref[...]
    wide = tokens.astype(jnp.float32)
    fresh_gate = jax.nn.log_sigmoid(
        jnp.concatenate(
            [
                jnp.sum(wide * forget_ref[j:j + 1, :].astype(jnp.float32), axis=1, keepdims=True)
                for j in range(kv_count)
            ],
            axis=1,
        )
    )
    waits["keys"]()
    fresh_key = jnp.dot(tokens, key_weight_ref[...], preferred_element_type=jnp.float32)
    fresh_key = fresh_key.astype(jnp.bfloat16).astype(jnp.float32)
    fresh_value = jnp.dot(tokens, value_weight_ref[...], preferred_element_type=jnp.float32)
    fresh_value = fresh_value.astype(jnp.bfloat16).astype(jnp.float32)
    pieces = waits["pieces"]
    piece = model // pieces
    for i in range(pieces):
        waits["query"](i)
        part = jnp.dot(
            tokens, query_weight_ref[:, i * piece:(i + 1) * piece], preferred_element_type=jnp.float32
        ).astype(jnp.bfloat16).astype(jnp.float32)
        for h in range(piece // head_dim):
            head = i * (piece // head_dim) + h
            group = head // grouped
            fields = [jnp.zeros((seqs, head_dim), jnp.float32)] * kv_count
            fields[group] = part[:, h * head_dim:(h + 1) * head_dim]
            query_ref[head * seqs:(head + 1) * seqs, :] = jnp.concatenate(fields, axis=1)
    waits["caches"]()
    positions = lax.broadcasted_iota(jnp.int32, (kv_count, cache_len), 1)
    row_group = lax.broadcasted_iota(jnp.int32, (heads, 1), 0) // grouped
    for b in range(seqs):
        length = lengths_ref[b]
        gates = gates_ref[b]
        latest = jnp.sum(jnp.where(positions == length - 1, gates, 0.0), axis=1, keepdims=True)
        offsets = jnp.where(positions < length, latest - gates, -jnp.inf)
        spread = offsets[0:1] + fresh_gate[b:b + 1, 0:1]
        spread = jnp.broadcast_to(spread, (heads, cache_len))
        for j in range(1, kv_count):
            spread = jnp.where(row_group == j, offsets[j:j + 1] + fresh_gate[b:b + 1, j:j + 1], spread)
        queries = query_ref[pl.ds(b, heads, stride=seqs), :]
        past = lax.dot_general(
            queries.astype(jnp.bfloat16), keys_ref[b], (((1,), (1,)), ((), ())),
            preferred_element_type=jnp.float32,
        )
        past = past * ratio_value + spread
        self_part = ratio_value * jnp.sum(queries * fresh_key[b:b + 1], axis=1, keepdims=True)
        highest = jnp.maximum(jnp.max(past, axis=1, keepdims=True), self_part)
        past_exp = jnp.exp(past - highest)
        own_exp = jnp.exp(self_part - highest)
        denominator = jnp.sum(past_exp, axis=1, keepdims=True) + own_exp
        past_weight = (past_exp / denominator).astype(jnp.bfloat16)
        own_weight = (own_exp / denominator).astype(jnp.bfloat16).astype(jnp.float32)
        mixed = jnp.dot(past_weight, values_ref[b], preferred_element_type=jnp.float32)
        mixed = mixed + own_weight * fresh_value[b:b + 1]
        rows_ref[pl.ds(b, heads, stride=seqs), :] = mixed
        waits["after"](b)
    fields = []
    for h in range(heads):
        group = h // grouped
        fields.append(rows_ref[h * seqs:(h + 1) * seqs, group * head_dim:(group + 1) * head_dim])
    return jnp.concatenate(fields, axis=1).astype(jnp.bfloat16)


def kernel(
    widths, heads,
    tokens_ref, gates_ref, lengths_ref, forget_ref, gain_ref, bias_ref, scale_ref,
    routes_ref, shares_ref, query_hbm, key_hbm, value_hbm, keys_hbm, values_hbm, out_hbm,
    gate_hbm, up_hbm, down_hbm, dense_gate_hbm, dense_up_hbm, dense_down_hbm,
    result_ref, *scratch,
):
    pool = list(scratch)
    take = lambda amount: [pool.pop(0) for _ in range(amount)]
    gate_ref, up_ref, down_ref, dense_gate_ref, dense_up_ref, dense_down_ref = take(6)
    load_sem, swap_send, swap_recv = take(3)
    query_weight_ref, key_weight_ref, value_weight_ref, keys_ref, values_ref, early_sem = take(6)
    query_ref, attended_rows_ref, share_ref, rows_ref, hidden_ref, dense_ref, settled_ref = take(7)
    dense_in_ref, dense_out_ref = take(2)
    slab_refs = take(2)
    slab_own, scatter_send, scatter_recv, slab_send, slab_recv, twin_send, twin_recv = take(7)
    queue_ref, queue_send, queue_recv, back_ref, back_in_ref, back_send, back_recv = take(7)
    chunks = len(widths)
    gathered = take(chunks)
    gather_send, gather_recv = take(2)
    per_chunk = []
    for _ in range(chunks):
        per_chunk.append((take(1)[0], take(AXES), take(AXES - 1)))
    reduce_send, reduce_recv = take(2)
    total_rows, model = rows_ref.shape
    seqs = tokens_ref.shape[0]
    slab = model // RING
    half = slab // 2

    me = lax.axis_index("ep")
    core = lax.rem(me, 2)
    twin = me + 1 - 2 * core
    coords, strides, rest, stride = [], [], me // 2, 2
    for _ in range(AXES):
        coords.append(lax.rem(rest, RING))
        strides.append(stride)
        rest = rest // RING
        stride *= RING
    x, y, z = coords

    def partner(axis, k):
        other = lax.rem(coords[axis] + k, RING)
        return other, me + (other - coords[axis]) * strides[axis]

    def remote(source, target, send, recv, device):
        return pltpu.make_async_remote_copy(
            src_ref=source, dst_ref=target, send_sem=send, recv_sem=recv,
            device_id=(device,), device_id_type=MESH,
        )

    barrier = pltpu.get_barrier_semaphore()
    pl.semaphore_signal(barrier, inc=1, device_id=(twin,), device_id_type=MESH)
    for axis in range(AXES):
        for k in range(1, RING):
            pl.semaphore_signal(
                barrier, inc=1, device_id=(partner(axis, k)[1],), device_id_type=MESH
            )

    pieces = 4
    piece = model // pieces
    early = [
        pltpu.make_async_copy(source, target, early_sem.at[i])
        for i, (source, target) in enumerate(
            [(key_hbm, key_weight_ref), (value_hbm, value_weight_ref)]
            + [
                (
                    query_hbm.at[:, pl.ds(i * piece, piece)],
                    query_weight_ref.at[:, pl.ds(i * piece, piece)],
                )
                for i in range(pieces)
            ]
            + [(keys_hbm, keys_ref), (values_hbm, values_ref)]
        )
    ]
    own_slabs = [
        pltpu.make_async_copy(
            out_hbm.at[:, pl.ds(pl.multiple_of(x * slab + c * half, half), half)],
            slab_refs[c].at[z, y, x, core], slab_own.at[c],
        )
        for c in range(2)
    ]
    for copy in own_slabs:
        copy.start()
    for copy in early:
        copy.start()
    pl.semaphore_wait(barrier, 1 + AXES * (RING - 1))

    scatter = []
    for k in range(1, RING):
        other, device = partner(0, k)
        for c in range(2):
            scatter.append(
                remote(
                    out_hbm.at[:, pl.ds(pl.multiple_of(other * slab + c * half, half), half)],
                    slab_refs[c].at[z, y, x, core],
                    scatter_send.at[c, k - 1], scatter_recv.at[c, k - 1], device,
                )
            )
    for copy in scatter:
        copy.start()

    sources = (gate_hbm, up_hbm, down_hbm, dense_gate_hbm, dense_up_hbm, dense_down_hbm)
    targets = (gate_ref, up_ref, down_ref, dense_gate_ref, dense_up_ref, dense_down_ref)
    loads = [
        pltpu.make_async_copy(source, target.at[0], load_sem.at[i])
        for i, (source, target) in enumerate(zip(sources, targets))
    ]
    swaps = [
        remote(source, target.at[1], swap_send.at[i], swap_recv.at[i], twin)
        for i, (source, target) in enumerate(zip(sources, targets))
    ]

    slab_orders = [[1, 2], [2, 1]]
    slab_have = [[], []]
    slab_flying = [[], []]
    twins = []

    def slab_at(c, fixed):
        at = [fixed.get(axis, slice(None)) for axis in (2, 1)]
        return slab_refs[c].at[at[0], at[1], :, core]

    def to_twin(c, number, block):
        copy = remote(block, block, twin_send.at[c, number], twin_recv.at[c, number], twin)
        copy.start()
        twins.append(copy)

    def slab_launch(c, stage):
        axis = slab_orders[c][stage]
        fixed = {other: coords[other] for other in (1, 2) if other not in slab_have[c]}
        copies = []
        for k in range(1, RING):
            copy = remote(
                slab_at(c, fixed), slab_at(c, fixed),
                slab_send.at[c, stage, k - 1], slab_recv.at[c, stage, k - 1], partner(axis, k)[1],
            )
            copy.start()
            copies.append(copy)
        slab_flying[c] = copies

    def slab_land(c, stage):
        axis = slab_orders[c][stage]
        for k, copy in enumerate(slab_flying[c], 1):
            copy.wait()
            fixed = {other: coords[other] for other in (1, 2) if other not in slab_have[c]}
            fixed[axis] = lax.rem(coords[axis] + RING - k, RING)
            to_twin(c, 1 + stage * (RING - 1) + k - 1, slab_at(c, fixed))
        slab_have[c].append(axis)

    def slabs_begin():
        for copy in own_slabs:
            copy.wait()
        for copy in scatter:
            copy.wait()
        for c in range(2):
            slab_launch(c, 0)
        for c in range(2):
            to_twin(c, 0, slab_at(c, {1: y, 2: z}))

    def slabs_second():
        for c in range(2):
            slab_land(c, 0)
            slab_launch(c, 1)

    def wait_all(some):
        for copy in some:
            copy.wait()

    def wait_query(i):
        early[2 + i].wait()
        if i == pieces - 1:
            slabs_begin()

    def wait_caches():
        for copy in loads + swaps:
            copy.start()
        wait_all(early[2 + pieces:])

    def after(b):
        if b == 1:
            slabs_second()

    waits = {
        "keys": lambda: wait_all(early[:2]),
        "query": wait_query,
        "pieces": pieces,
        "caches": wait_caches,
        "after": after,
    }
    kv_count = gates_ref.shape[1]
    attended = attend(
        heads, kv_count, tokens_ref, query_weight_ref, key_weight_ref, value_weight_ref,
        forget_ref, keys_ref, values_ref, gates_ref, lengths_ref, query_ref,
        attended_rows_ref, waits,
    )
    queue_ref[x] = attended
    queued = []
    for k in range(1, RING):
        copy = remote(
            queue_ref.at[x], queue_ref.at[x], queue_send.at[k - 1], queue_recv.at[k - 1],
            partner(0, k)[1],
        )
        copy.start()
        queued.append(copy)

    own_expert = me // (2 * RING ** AXES // EXPERTS)
    share_tile = 16 * seqs
    chosen = jnp.sum(
        jnp.where(routes_ref[...] == own_expert, shares_ref[...], 0.0), axis=0, keepdims=True
    )
    row = lax.broadcasted_iota(jnp.int32, (share_tile, 2 * share_tile), 0)
    lane = lax.broadcasted_iota(jnp.int32, (share_tile, 2 * share_tile), 1)
    wanted = lane == (row // seqs) * (2 * seqs) + core * seqs + lax.rem(row, seqs)
    for i in range(total_rows // share_tile):
        share_ref[i * share_tile:(i + 1) * share_tile, :] = jnp.sum(
            jnp.where(wanted, chosen[:, 2 * i * share_tile:2 * (i + 1) * share_tile], 0.0),
            axis=1, keepdims=True,
        )

    for c in range(2):
        slab_land(c, 1)
    wait_all(queued)
    wait_all(twins)
    lines = queue_ref[...].astype(jnp.float32).reshape(RING * seqs, model).astype(jnp.bfloat16)
    for c in range(2):
        part = jnp.dot(
            lines, slab_refs[c][...].reshape(model, half), preferred_element_type=jnp.float32
        )
        back_ref[:, :, c * half:(c + 1) * half] = part.reshape(RING, seqs, half)
    back_in_ref[x] = back_ref[x]
    returned = []
    for k in range(1, RING):
        other, device = partner(0, k)
        copy = remote(
            back_ref.at[other], back_in_ref.at[x], back_send.at[k - 1], back_recv.at[k - 1], device
        )
        copy.start()
        returned.append(copy)

    wait_all(loads)
    wait_all(swaps)
    units = dense_gate_ref.shape[1]
    pitch = (units + 15) // 16 * 16
    room = dense_out_ref.shape[0]
    gap = jnp.zeros((pitch - units, model), jnp.float32)
    rest = jnp.zeros((room - 2 * pitch, model), jnp.float32)

    def packed(ref):
        return jnp.concatenate(
            [ref[0].astype(jnp.float32), gap, ref[1].astype(jnp.float32), gap, rest], axis=0
        ).astype(jnp.bfloat16)

    dense_in_ref[:room, :] = packed(dense_gate_ref)
    dense_in_ref[room:, :] = packed(dense_up_ref)
    dense_out_ref[...] = packed(dense_down_ref)

    wait_all(returned)
    projected = jnp.concatenate([back_in_ref[i] for i in range(RING)], axis=1)
    settled = layer_norm(
        residual_scale * tokens_ref[...].astype(jnp.float32) + projected, gain_ref[0:1], bias_ref[0:1]
    )
    settled_ref[...] = settled

    orders = [[(c + stage) % AXES for stage in range(AXES)] for c in range(chunks)]
    begin = 0
    for c in range(chunks):
        gathered[c][z, y, x] = settled[:, begin:begin + widths[c]]
        begin += widths[c]
    flying = [None] * chunks
    have = [[] for _ in orders]

    def spread(c, stage):
        axis = orders[c][stage]
        index = tuple(
            slice(None) if other in have[c] else coords[other] for other in range(AXES)[::-1]
        )
        copies = []
        for k in range(1, RING):
            copy = remote(
                gathered[c].at[index], gathered[c].at[index],
                gather_send.at[c, stage, k - 1], gather_recv.at[c, stage, k - 1],
                partner(axis, k)[1],
            )
            copy.start()
            copies.append(copy)
        flying[c] = copies
        have[c].append(axis)

    for c in range(chunks):
        spread(c, 0)
    for stage in range(AXES):
        for c in range(chunks):
            wait_all(flying[c])
            if stage < AXES - 1:
                spread(c, stage + 1)
    begin = 0
    for c in range(chunks):
        block = gathered[c][...].astype(jnp.float32).reshape(total_rows, widths[c])
        rows_ref[:, begin:begin + widths[c]] = block.astype(jnp.bfloat16)
        begin += widths[c]

    tile = 256
    tiles = total_rows // tile
    span = 256
    contract = (((1,), (1,)), ((), ()))

    @pl.loop(0, tiles)
    def _(row):
        at_rows = pl.ds(pl.multiple_of(row * tile, tile), tile)
        inputs = rows_ref[at_rows, :]
        both = lax.dot_general(inputs, dense_in_ref[...], contract, preferred_element_type=jnp.float32)
        dense_ref[at_rows, :] = (jax.nn.silu(both[:, :room]) * both[:, room:]).astype(jnp.bfloat16)

        @pl.loop(0, 2)
        def _(side):
            gate_val = lax.dot_general(
                rows_ref[at_rows, :], gate_ref[side], contract, preferred_element_type=jnp.float32
            )
            up_val = lax.dot_general(
                rows_ref[at_rows, :], up_ref[side], contract, preferred_element_type=jnp.float32
            )
            hidden_ref[side, at_rows, :] = (jax.nn.silu(gate_val) * up_val).astype(jnp.bfloat16)

    def at_axis(left, axis, index):
        return tuple(index if other == axis else slice(None) for other in left)

    current = [entry[0] for entry in per_chunk]
    left = [list(range(AXES))[::-1] for _ in orders]
    sending = [None] * chunks
    finished = [None] * chunks

    def launch(c, stage):
        axis = orders[c][stage]
        copies = []
        for k in range(1, RING):
            other, device = partner(axis, k)
            copy = remote(
                current[c].at[at_axis(left[c], axis, other)], per_chunk[c][1][stage].at[k - 1],
                reduce_send.at[c, stage, k - 1], reduce_recv.at[c, stage, k - 1], device,
            )
            copy.start()
            copies.append(copy)
        sending[c] = copies

    def advance(c, stage):
        axis = orders[c][stage]
        wait_all(sending[c])
        landed = per_chunk[c][1][stage]
        own = current[c][at_axis(left[c], axis, coords[axis])].astype(jnp.float32)
        for k in range(RING - 1):
            own = own + landed[k].astype(jnp.float32)
        left[c] = [other for other in left[c] if other != axis]
        if stage == AXES - 1:
            finished[c] = own
        else:
            current[c] = per_chunk[c][2][stage]
            current[c][...] = own.astype(jnp.bfloat16)
            launch(c, stage + 1)

    tile_lead = tile // seqs // (RING * RING)
    begin = 0
    for c in range(chunks):
        span = 128 if widths[c] % 256 else 256
        steps = widths[c] // span

        @pl.loop(0, tiles * steps)
        def _(step):
            row = step // steps
            column = pl.multiple_of(lax.rem(step, steps) * span, span)
            at_columns = pl.ds(pl.multiple_of(begin + column, span), span)
            at_rows = pl.ds(pl.multiple_of(row * tile, tile), tile)
            expert_out = jnp.dot(
                hidden_ref[0, at_rows, :], down_ref[0, :, at_columns], preferred_element_type=jnp.float32
            ) + jnp.dot(
                hidden_ref[1, at_rows, :], down_ref[1, :, at_columns], preferred_element_type=jnp.float32
            )
            dense_out = jnp.dot(
                dense_ref[at_rows, :], dense_out_ref[:, at_columns], preferred_element_type=jnp.float32
            )
            part = share_ref[at_rows, :] * expert_out + scale_ref[:, at_columns] * dense_out
            per_chunk[c][0][pl.ds(row * tile_lead, tile_lead), :, :, :, pl.ds(column, span)] = part.reshape(
                tile_lead, RING, RING, seqs, span
            ).astype(jnp.bfloat16)

        begin += widths[c]
        launch(c, 0)

    for stage in range(AXES):
        for c in range(chunks):
            advance(c, stage)
    ffn = jnp.concatenate(finished, axis=-1)
    result_ref[...] = layer_norm(
        residual_scale * settled_ref[...].astype(jnp.float32) + ffn, gain_ref[1:2], bias_ref[1:2]
    )


def whole_step(
    heads, tokens, gates, lengths, forget, norm_gain, norm_bias, dense_scale, routes, shares,
    query_weight, key_weight, value_weight, cache_keys, cache_values, out_weight,
    expert_gate, expert_up, expert_down, dense_gate, dense_up, dense_down,
):
    seqs, model = tokens.shape
    widths = [768, 640, 640]
    chips = RING ** AXES
    total_rows = chips * seqs
    lead = (RING,) * AXES
    half = model // RING // 2
    bf16 = jnp.bfloat16
    dma = pltpu.SemaphoreType.DMA
    room = 128
    scratch = [
        pltpu.VMEM((2,) + array.shape, array.dtype)
        for array in (expert_gate, expert_up, expert_down, dense_gate, dense_up, dense_down)
    ]
    scratch += [dma((6,)), dma((6,)), dma((6,))]
    scratch += [
        pltpu.VMEM(array.shape, array.dtype)
        for array in (query_weight, key_weight, value_weight, cache_keys, cache_values)
    ]
    scratch += [
        dma((8,)),
        pltpu.VMEM((heads * seqs, key_weight.shape[1]), jnp.float32),
        pltpu.VMEM((heads * seqs, key_weight.shape[1]), jnp.float32),
        pltpu.VMEM((total_rows, 1), jnp.float32),
        pltpu.VMEM((total_rows, model), bf16),
        pltpu.VMEM((2, total_rows, expert_gate.shape[0]), bf16),
        pltpu.VMEM((total_rows, room), bf16),
        pltpu.VMEM((seqs, model), bf16),
        pltpu.VMEM((2 * room, model), bf16),
        pltpu.VMEM((room, model), bf16),
    ]
    scratch += [pltpu.VMEM((RING, RING, RING, 2, out_weight.shape[0], half), bf16)] * 2
    scratch += [
        dma((2,)), dma((2, RING - 1)), dma((2, RING - 1)),
        dma((2, 2, RING - 1)), dma((2, 2, RING - 1)), dma((2, 7)), dma((2, 7)),
        pltpu.VMEM((RING, seqs, model), bf16), dma((RING - 1,)), dma((RING - 1,)),
        pltpu.VMEM((RING, seqs, model // RING), jnp.float32),
        pltpu.VMEM((RING, seqs, model // RING), jnp.float32),
        dma((RING - 1,)), dma((RING - 1,)),
    ]
    scratch += [pltpu.VMEM(lead + (seqs, width), bf16) for width in widths]
    scratch += [dma((len(widths), AXES, RING - 1))] * 2
    for width in widths:
        scratch.append(pltpu.VMEM(lead + (seqs, width), bf16))
        scratch += [
            pltpu.VMEM((RING - 1,) + (RING,) * rest + (seqs, width), bf16) for rest in (2, 1, 0)
        ]
        scratch += [pltpu.VMEM((RING,) * rest + (seqs, width), bf16) for rest in (2, 1)]
    scratch += [dma((len(widths), AXES, RING - 1))] * 2
    vmem = pl.BlockSpec(memory_space=pltpu.VMEM)
    away = pl.BlockSpec(memory_space=pl.ANY)
    return pl.pallas_call(
        functools.partial(kernel, widths, heads),
        out_shape=jax.ShapeDtypeStruct((seqs, model), jnp.bfloat16),
        in_specs=[vmem] * 2
        + [pl.BlockSpec(memory_space=pltpu.SMEM)]
        + [vmem] * 6
        + [away] * 12,
        out_specs=vmem,
        scratch_shapes=scratch,
        compiler_params=pltpu.CompilerParams(
            collective_id=0, has_side_effects=True, vmem_limit_bytes=60 * 1024 * 1024
        ),
        name="whole_step",
    )(
        tokens, gates, lengths, forget, norm_gain, norm_bias, dense_scale, routes, shares,
        query_weight, key_weight, value_weight, cache_keys, cache_values, out_weight,
        expert_gate, expert_up, expert_down, dense_gate, dense_up, dense_down,
    )


def local(
    tokens,
    cache_keys,
    cache_values,
    cum_gates,
    lengths,
    query_weight,
    key_weight,
    value_weight,
    forget_weight,
    out_weight,
    norm_gain,
    norm_bias,
    dense_gate_weight,
    dense_up_weight,
    dense_down_weight,
    dense_scale,
    expert_gate_weight,
    expert_up_weight,
    expert_down_weight,
    routes,
    route_weights,
):
    head_dim = key_weight.shape[1] // cum_gates.shape[2]
    heads = query_weight.shape[1] // head_dim
    return whole_step(
        heads, tokens, jnp.transpose(cum_gates, (0, 2, 1)), lengths, forget_weight.T,
        norm_gain, norm_bias, dense_scale[None, :], routes.T, route_weights.T,
        query_weight, key_weight, value_weight, cache_keys, cache_values, out_weight,
        expert_gate_weight.T, expert_up_weight.T, expert_down_weight,
        dense_gate_weight.T, dense_up_weight.T, dense_down_weight,
    )


def solution(mesh):
    return jax.shard_map(
        local,
        mesh=mesh,
        in_specs=(
            P("ep", None),
            P("ep", None, None),
            P("ep", None, None),
            P("ep", None, None),
            P("ep"),
            P(),
            P(),
            P(),
            P(),
            P("ep", None),
            P(),
            P(),
            P(None, "ep"),
            P(None, "ep"),
            P("ep", None),
            P(),
            P(None, "ep"),
            P(None, "ep"),
            P("ep", None),
            P(),
            P(),
        ),
        out_specs=P("ep", None),
        check_vma=False,
    )
```
